32 devices in a mesh: ep: 8 (over z, x), tp: 4 (over y, core).
Axes of the slice: x: 2, y: 2, z: 4, core: 2. Of those that a mesh axis runs over, the one named last changes fastest.
Arguments:
- mixer_input: bfloat16 [4096, 2048], P(('ep', 'tp')), may hold values from -6 to 6
- log_decay: float32 [4096, 8], P('ep', 'tp'), may hold values from -0.8 to 0
- mixer_gain: float32 [2048], replicated, may hold values from 0.1 to 1.9
- query_weight: bfloat16 [2048, 1024], P(None, 'tp'), may hold values from -0.125 to 0.125
- key_weight: bfloat16 [2048, 1024], P(None, 'tp'), may hold values from -0.125 to 0.125
- value_weight: bfloat16 [2048, 2048], P(None, 'tp'), may hold values from -0.125 to 0.125
- gate_weight: bfloat16 [2048, 2048], P(None, 'tp'), may hold values from -0.125 to 0.125
- head_gain: float32 [2048], P('tp'), may hold values from 0.1 to 1.9
- output_weight: bfloat16 [2048, 2048], P('tp'), may hold values from -0.125 to 0.125
- expert_input: bfloat16 [4096, 2048], P(('ep', 'tp')), may hold values from -6 to 6
- expert_gain: float32 [2048], replicated, may hold values from 0.1 to 1.9
- routes: int32 [4096, 2], P(('ep', 'tp')), may hold values from 0 to 31, as said below
- group_weight: float32 [4096], P(('ep', 'tp')), may hold values from 0.3 to 1
- pair_weight: float32 [4096, 2], P(('ep', 'tp')), may hold values from 0.2 to 1
- expert_gate: bfloat16 [32, 2048, 1024], P(('ep', 'tp')), may hold values from -0.125 to 0.125
- expert_up: bfloat16 [32, 2048, 1024], P(('ep', 'tp')), may hold values from -0.125 to 0.125
- expert_down: bfloat16 [32, 1024, 2048], P(('ep', 'tp')), may hold values from -0.1875 to 0.1875
Outputs:
- mixer_output: bfloat16 [4096, 2048], P(('ep', 'tp'))
- expert_output: bfloat16 [4096, 2048], P(('ep', 'tp'))
The draws below stay inside these ranges and needn't reach their ends.
Inputs may be any that keep to these rules, and one draw needn't show every extreme that they name: `routes`: in the rows of one device each expert is named at most 12 times; one expert is named exactly 12 times in the rows of every device. A row names two different experts of the same group, a group being 8 consecutive expert numbers.
All inputs are finite; a program needn't handle non-finite values.
Results may differ from the reference program's by a relative error of at most 0.023.
Values may be sent and summed in bfloat16 or wider, within the bound.
A program may use at most 128 MiB of HBM per device.

```python
import jax
import jax.numpy as jnp
from jax import lax

D = 2048
RETENTION_HEADS = 8
KEY_DIM = 128
VALUE_DIM = 256
SPAN = 512
FF = 1024
GROUPS = 4
TOPK = 2
TOK_B = 128
KEY_WIDTH = 1024
VALUE_WIDTH = 2048
SEG_ROWS = 512
FIRST_POSITIONS = 4096
TOKENS_B = 4096
EXPERTS = 32
GROUP_SIZE = 8
CAP = 12
N_EP = 8
N_TP = 4


def draw_log_decay(key, part):
    split_random_keys = jax.random.split(jax.random.fold_in(key, 3), 7)
    fast_share = 0.5
    fast_heads = jax.random.uniform(split_random_keys[0], (RETENTION_HEADS,)) < fast_share
    fast_rate = 1.0 / jax.random.uniform(split_random_keys[1], (RETENTION_HEADS,), minval=30.0, maxval=100.0)
    slow_rate = jax.random.uniform(split_random_keys[2], (RETENTION_HEADS,), minval=0.1, maxval=0.5) / FIRST_POSITIONS
    head_rate = jnp.where(fast_heads, fast_rate, slow_rate)
    segments = FIRST_POSITIONS // SEG_ROWS
    segment_scale = jnp.exp(jax.random.uniform(split_random_keys[3], (segments,), minval=-0.7, maxval=0.7))
    row_scale = jnp.repeat(segment_scale, SEG_ROWS)
    jitter = jax.random.uniform(split_random_keys[4], (FIRST_POSITIONS, RETENTION_HEADS), minval=0.5, maxval=1.5)
    decay_factor = -head_rate[None, :] * row_scale[:, None] * jitter
    spike_rows = jax.random.randint(split_random_keys[5], (2,), 0, FIRST_POSITIONS)
    spike_loss = jnp.log(jax.random.uniform(split_random_keys[6], (2, RETENTION_HEADS), minval=0.5, maxval=0.8))
    position_list = jnp.arange(FIRST_POSITIONS)
    for index_value in range(2):
        decay_factor = decay_factor + jnp.where(position_list[:, None] == spike_rows[index_value], spike_loss[index_value][None, :], 0.0)
    return decay_factor.astype(jnp.float32)


def draw_routes(key, part):
    base_key = jax.random.fold_in(key, 7)
    chosen_key, block_base = jax.random.split(base_key)
    full_expert = jax.random.randint(chosen_key, (), 0, EXPERTS)
    pair_count = EXPERTS // 2

    def one_block(block_key):
        split_random_keys = jax.random.split(block_key, GROUPS + 3)
        orders = jnp.stack([jax.random.permutation(split_random_keys[group], GROUP_SIZE) for group in range(GROUPS)])
        labels = (orders + GROUP_SIZE * jnp.arange(GROUPS)[:, None]).reshape(-1).astype(jnp.int32)
        location = jnp.argmax(labels == full_expert)
        full_pair = location // 2
        slot_pairs = jnp.repeat(jnp.arange(pair_count), CAP)
        rank_order = jax.random.permutation(split_random_keys[GROUPS], pair_count * CAP)
        scores = jnp.where(slot_pairs == full_pair, rank_order, rank_order + pair_count * CAP)
        picked = jnp.argsort(scores)[:TOK_B]
        token_pairs = slot_pairs[picked][jax.random.permutation(split_random_keys[GROUPS + 1], TOK_B)]
        swapped = jax.random.randint(split_random_keys[GROUPS + 2], (TOK_B,), 0, 2)
        first_id = labels[2 * token_pairs + swapped]
        second = labels[2 * token_pairs + 1 - swapped]
        return jnp.stack([first_id, second], axis=1)
    block_keys = jax.random.split(block_base, TOKENS_B // TOK_B)
    return jax.vmap(one_block)(block_keys).reshape(TOKENS_B, TOPK).astype(jnp.int32)


def block_levels(key, extent, cuts, smallest, top_value):
    def one(dim, parts):
        draws = jax.random.uniform(jax.random.fold_in(jax.random.fold_in(key, 6), dim), (parts,), jnp.float32, smallest / len(cuts), top_value / len(cuts))
        return jnp.repeat(jnp.exp(draws), extent[dim] // parts).reshape((-1,) + (1,) * (len(extent) - dim - 1))

    loudness = one(*cuts[0])
    for cut in cuts[1:]:
        loudness = loudness * one(*cut)
    return loudness


def noise(key, shape, scale, reach, cuts=(), held_as=jnp.bfloat16):
    entries = jax.random.normal(key, shape, jnp.float32) * scale
    if len(cuts) > 0:
        entries = block_levels(key, shape, cuts, -0.22, 0.18) * entries
    return jnp.clip(entries, min=-reach, max=reach).astype(held_as)


def setup_inputs(seed: int = 0) -> dict:
    arg_keys = jax.random.split(jax.random.key(seed), 18)
    mixer_input = noise(arg_keys[0], (FIRST_POSITIONS, D), 1.0, 6.0, ((0, 32),))
    log_decay = draw_log_decay(jax.random.fold_in(arg_keys[17], 71), 0)
    mixer_gain = jnp.clip(1.0 + 0.18 * jax.random.normal(arg_keys[2], (D,), jnp.float32), 0.1, 1.9)
    query_weight = noise(arg_keys[3], (D, KEY_WIDTH), D ** -0.5, 0.125, ((1, 4),))
    key_weight = noise(arg_keys[4], (D, KEY_WIDTH), D ** -0.5, 0.125, ((1, 4),))
    value_weight = noise(arg_keys[5], (D, VALUE_WIDTH), D ** -0.5, 0.125, ((1, 4),))
    gate_weight = noise(arg_keys[6], (D, VALUE_WIDTH), D ** -0.5, 0.125, ((1, 4),))
    head_gain = jnp.clip(1.0 + 0.18 * jax.random.normal(arg_keys[7], (VALUE_WIDTH,), jnp.float32), 0.1, 1.9)
    output_weight = noise(arg_keys[8], (VALUE_WIDTH, D), VALUE_WIDTH ** -0.5, 0.125, ((0, 4),))
    expert_input = noise(arg_keys[9], (TOKENS_B, D), 1.0, 6.0, ((0, 32),))
    expert_gain = jnp.clip(1.0 + 0.18 * jax.random.normal(arg_keys[10], (D,), jnp.float32), 0.1, 1.9)
    routes = draw_routes(jax.random.fold_in(arg_keys[17], 71), 0)
    group_weight = jnp.clip(0.3 + 0.7 * jax.random.uniform(arg_keys[12], (TOKENS_B,), jnp.float32) ** block_levels(arg_keys[12], (TOKENS_B,), ((0, 32),), -0.2, 0.2), 0.3, 1.0)
    pair_weight = jnp.clip(0.2 + 0.8 * jax.random.uniform(arg_keys[13], (TOKENS_B, TOPK), jnp.float32) ** block_levels(arg_keys[13], (TOKENS_B, TOPK), ((0, 32),), -0.2, 0.2), 0.2, 1.0)
    expert_gate = noise(arg_keys[14], (EXPERTS, D, FF), D ** -0.5, 0.125, ((0, 32),))
    expert_up = noise(arg_keys[15], (EXPERTS, D, FF), D ** -0.5, 0.125, ((0, 32),))
    expert_down = noise(arg_keys[16], (EXPERTS, FF, D), FF ** -0.5, 0.1875, ((0, 32),))
    return dict(mixer_input=mixer_input, log_decay=log_decay, mixer_gain=mixer_gain, query_weight=query_weight, key_weight=key_weight, value_weight=value_weight, gate_weight=gate_weight, head_gain=head_gain, output_weight=output_weight, expert_input=expert_input, expert_gain=expert_gain, routes=routes, group_weight=group_weight, pair_weight=pair_weight, expert_gate=expert_gate, expert_up=expert_up, expert_down=expert_down)


EPSILON = 1e-05
THETA = 10000.0

def layer_norm(matrix, norm_gain):
    matrix = matrix.astype(jnp.float32)
    average = lax.optimization_barrier(jnp.mean(matrix, axis=-1, keepdims=True))
    centred = matrix - average
    spread = lax.optimization_barrier(jnp.mean(centred * centred, axis=-1, keepdims=True))
    return centred * lax.rsqrt(spread + EPSILON) * norm_gain.astype(jnp.float32)

def rotate(values, position):
    halfway = values.shape[-1] // 2
    frequency = THETA ** (-jnp.arange(halfway, dtype=jnp.float32) / halfway)
    angles = position[:, None] * frequency[None, :]
    cosine = jnp.cos(angles)[:, None, :]
    sine_part = jnp.sin(angles)[:, None, :]
    leading = values[..., :halfway]
    trailing = values[..., halfway:]
    return jnp.concatenate([leading * cosine - trailing * sine_part, trailing * cosine + leading * sine_part], axis=-1)

def block_step(state, inputs):
    query_rows, key_rows, value_rows, decay_factor = inputs
    span_len = query_rows.shape[0]
    cumulative = jnp.cumsum(decay_factor, axis=0)
    causal = jnp.arange(span_len)[:, None] >= jnp.arange(span_len)[None, :]
    log_gaps = cumulative.T[:, :, None] - cumulative.T[:, None, :]
    weight = jnp.where(causal[None], jnp.exp(jnp.minimum(log_gaps, 0.0)), 0.0)
    query_float = query_rows.astype(jnp.float32)
    key_float = key_rows.astype(jnp.float32)
    value_float = value_rows.astype(jnp.float32)
    scores = jnp.einsum('thd,shd->hts', query_float, key_float, precision=lax.Precision.HIGHEST)
    decayed = (scores * weight).astype(jnp.bfloat16).astype(jnp.float32)
    within = jnp.einsum('hts,she->the', decayed, value_float, precision=lax.Precision.HIGHEST)
    scaled = query_float * jnp.exp(cumulative)[:, :, None]
    carried = jnp.einsum('thd,hde->the', scaled, state, precision=lax.Precision.HIGHEST)
    span_total = cumulative[-1]
    remain = jnp.exp(span_total[None, :] - cumulative)
    update = jnp.einsum('shd,she->hde', key_float * remain[:, :, None], value_float, precision=lax.Precision.HIGHEST)
    return (state * jnp.exp(span_total)[:, None, None] + update, within + carried)

def token_mixer(mixer_input, log_decay, mixer_gain, query_weight, key_weight, value_weight, gate_weight, head_gain, output_weight):
    normed = layer_norm(mixer_input, mixer_gain).astype(jnp.bfloat16)

    def project(weight):
        return jnp.dot(normed, weight, preferred_element_type=jnp.float32).astype(jnp.bfloat16)
    query = project(query_weight).reshape(FIRST_POSITIONS, RETENTION_HEADS, KEY_DIM)
    keys_all = project(key_weight).reshape(FIRST_POSITIONS, RETENTION_HEADS, KEY_DIM)
    value = project(value_weight).reshape(FIRST_POSITIONS, RETENTION_HEADS, VALUE_DIM)
    gate = project(gate_weight).astype(jnp.float32)
    position = jnp.arange(FIRST_POSITIONS).astype(jnp.float32)
    rot_query = rotate(query.astype(jnp.float32), position).astype(jnp.bfloat16)
    rot_key = rotate(keys_all.astype(jnp.float32), position).astype(jnp.bfloat16)
    blocks = FIRST_POSITIONS // SPAN

    def split_blocks(tensor):
        return tensor.reshape((blocks, SPAN) + tensor.shape[1:])
    state_zero = jnp.zeros((RETENTION_HEADS, KEY_DIM, VALUE_DIM), jnp.float32)
    _, retained = lax.scan(block_step, state_zero, (split_blocks(rot_query), split_blocks(rot_key), split_blocks(value), split_blocks(log_decay)))
    retained = retained.reshape(FIRST_POSITIONS, RETENTION_HEADS, VALUE_DIM)
    average = lax.optimization_barrier(jnp.mean(retained, axis=-1, keepdims=True))
    centred = retained - average
    spread = lax.optimization_barrier(jnp.mean(centred * centred, axis=-1, keepdims=True))
    normed_heads = centred * lax.rsqrt(spread + EPSILON) * head_gain.reshape(RETENTION_HEADS, VALUE_DIM).astype(jnp.float32)
    gated = (jax.nn.silu(gate) * normed_heads.reshape(FIRST_POSITIONS, VALUE_WIDTH)).astype(jnp.bfloat16)
    group_cols = VALUE_WIDTH // N_TP
    summed = jnp.zeros((FIRST_POSITIONS, D), jnp.float32)
    for group in range(N_TP):
        lower = group * group_cols
        share_term = jnp.dot(gated[:, lower:lower + group_cols], output_weight[lower:lower + group_cols], preferred_element_type=jnp.float32).astype(jnp.bfloat16)
        summed = summed + share_term.astype(jnp.float32)
    return summed.astype(jnp.bfloat16)

def expert_mixture(expert_input, expert_gain, routes, group_weight, pair_weight, expert_gate, expert_up, expert_down):
    normed = layer_norm(expert_input, expert_gain).astype(jnp.bfloat16)
    flat_routes = routes.reshape(-1).astype(jnp.int32)
    capacity_rows = N_EP * N_TP * CAP
    mixing = (group_weight[:, None] * pair_weight).reshape(-1).astype(jnp.float32)

    def one_expert(carry, expert_id):
        matches = flat_routes == expert_id
        hits = jnp.nonzero(matches, size=capacity_rows, fill_value=0)[0].astype(jnp.int32)
        present = (jnp.arange(capacity_rows) < jnp.sum(matches)).astype(jnp.float32)
        token_ids = (hits // TOPK).astype(jnp.int32)
        gathered = normed[token_ids]
        gate_part = jnp.dot(gathered, expert_gate[expert_id], preferred_element_type=jnp.float32)
        up_part = jnp.dot(gathered, expert_up[expert_id], preferred_element_type=jnp.float32)
        hidden = (jax.nn.silu(gate_part) * up_part).astype(jnp.bfloat16)
        result = jnp.dot(hidden, expert_down[expert_id], preferred_element_type=jnp.float32).astype(jnp.bfloat16)
        contribution = result.astype(jnp.float32) * (mixing[hits] * present)[:, None]
        return (carry.at[token_ids].add(contribution), None)
    total, _ = lax.scan(one_expert, jnp.zeros((TOKENS_B, D), jnp.float32), jnp.arange(EXPERTS, dtype=jnp.int32))
    return total.astype(jnp.bfloat16)

def reference(mixer_input, log_decay, mixer_gain, query_weight, key_weight, value_weight, gate_weight, head_gain, output_weight, expert_input, expert_gain, routes, group_weight, pair_weight, expert_gate, expert_up, expert_down):
    mixer_output = token_mixer(mixer_input, log_decay, mixer_gain, query_weight, key_weight, value_weight, gate_weight, head_gain, output_weight)
    expert_output = expert_mixture(expert_input, expert_gain, routes, group_weight, pair_weight, expert_gate, expert_up, expert_down)
    return (mixer_output, expert_output)
```

```python
import jax
import jax.numpy as jnp
from jax import lax
from jax.sharding import PartitionSpec as P

KEY_DIM = 128
VALUE_DIM = 256
TOPK = 2
GROUPS = 4
META = 128

EPSILON = 1e-05
THETA = 10000.0
AXES = ("ep", "tp")


def layer_norm(matrix, norm_gain):
    matrix = matrix.astype(jnp.float32)
    average = jnp.mean(matrix, axis=-1, keepdims=True)
    centred = matrix - average
    spread = jnp.mean(centred * centred, axis=-1, keepdims=True)
    return centred * lax.rsqrt(spread + EPSILON) * norm_gain


def rotate(values, cosine, sine):
    halfway = values.shape[-1] // 2
    leading = values[..., :halfway]
    trailing = values[..., halfway:]
    return jnp.concatenate(
        [leading * cosine - trailing * sine, trailing * cosine + leading * sine], axis=-1
    )


def flip(array, axis, count, mask):
    return lax.ppermute(array, axis, [(i, i ^ mask) for i in range(count)])


def later(array, count, step):
    return lax.ppermute(array, "ep", [(i, i + step) for i in range(count - step)])


def gather_rows(rows, tp_count):
    blocks = [rows] * tp_count
    for far in range(2, tp_count, 2):
        blocks[far] = flip(rows, "tp", tp_count, far)
    blocks[1] = flip(rows, "tp", tp_count, 1)
    for far in range(2, tp_count, 2):
        blocks[far + 1] = flip(blocks[far], "tp", tp_count, 1)
    return blocks


def scatter_sum(blocks, tp_count):
    total = blocks[0].astype(jnp.float32)
    pairs = [
        flip(blocks[far + 1], "tp", tp_count, 1) for far in range(2, tp_count, 2)
    ]
    partner = flip(blocks[1], "tp", tp_count, 1)
    arrived = []
    for place, far in enumerate(range(2, tp_count, 2)):
        both = blocks[far].astype(jnp.float32) + pairs[place].astype(jnp.float32)
        arrived.append(flip(both.astype(jnp.bfloat16), "tp", tp_count, far))
    total = total + partner.astype(jnp.float32)
    for part in arrived:
        total = total + part.astype(jnp.float32)
    return total.astype(jnp.bfloat16)


def token_mixer(
    mixer_input,
    log_decay,
    mixer_gain,
    query_weight,
    key_weight,
    value_weight,
    gate_weight,
    head_gain,
    output_weight,
):
    ep_count = lax.axis_size("ep")
    tp_count = lax.axis_size("tp")
    place = lax.axis_index("tp")
    own_rows = mixer_input.shape[0]
    seg_rows = own_rows * tp_count
    heads_dev = query_weight.shape[1] // KEY_DIM

    window = later(jnp.sum(log_decay, axis=0), ep_count, 1)
    windows = [window]
    covered = 1
    while covered * 2 < ep_count:
        window = window + later(window, ep_count, covered)
        windows.append(window)
        covered *= 2

    normed = layer_norm(mixer_input, mixer_gain).astype(jnp.bfloat16)
    gathered = jnp.concatenate(gather_rows(normed, tp_count), axis=0)

    row = jnp.arange(seg_rows, dtype=jnp.int32)
    offset = (row // own_rows ^ place) * own_rows + row % own_rows
    natural = jnp.arange(seg_rows, dtype=jnp.int32)
    reach = (natural[None, :] <= offset[:, None])
    causal = offset[:, None] >= offset[None, :]
    cumulative = [
        jnp.sum(jnp.where(reach, log_decay[:, h][None, :], 0.0), axis=1)
        for h in range(heads_dev)
    ]
    totals = jnp.sum(log_decay, axis=0)

    position = (lax.axis_index("ep") * seg_rows + offset).astype(jnp.float32)
    halfway = KEY_DIM // 2
    frequency = THETA ** (-jnp.arange(halfway, dtype=jnp.float32) / halfway)
    angles = position[:, None] * frequency[None, :]
    cosine = jnp.cos(angles)
    sine = jnp.sin(angles)

    def project(weight):
        return jnp.dot(gathered, weight, preferred_element_type=jnp.float32)

    keys = project(key_weight).astype(jnp.bfloat16)
    values = project(value_weight).astype(jnp.bfloat16)
    queries = project(query_weight).astype(jnp.bfloat16)
    gates = project(gate_weight).astype(jnp.bfloat16)

    states = []
    head_keys = []
    for h in range(heads_dev):
        key = rotate(
            keys[:, h * KEY_DIM : (h + 1) * KEY_DIM].astype(jnp.float32), cosine, sine
        ).astype(jnp.bfloat16)
        head_keys.append(key)
        remain = jnp.exp(totals[h] - cumulative[h])
        weighted = (key.astype(jnp.float32) * remain[:, None]).astype(jnp.bfloat16)
        states.append(
            lax.dot_general(
                weighted,
                values[:, h * VALUE_DIM : (h + 1) * VALUE_DIM],
                (((0,), (0,)), ((), ())),
                preferred_element_type=jnp.float32,
            )
        )
    state = jnp.stack(states).astype(jnp.bfloat16)

    incoming = later(state, ep_count, 1).astype(jnp.float32)
    covered = 1
    if ep_count > 2:
        second = later(state, ep_count, 2).astype(jnp.float32)
        incoming = incoming + jnp.exp(windows[0])[:, None, None] * second
        covered = 2
    step = 1
    while covered < ep_count - 1:
        earlier = later(incoming.astype(jnp.bfloat16), ep_count, covered).astype(jnp.float32)
        incoming = incoming + jnp.exp(windows[step])[:, None, None] * earlier
        covered *= 2
        step += 1
    incoming = incoming.astype(jnp.bfloat16)

    gated = []
    for h in range(heads_dev):
        query = rotate(
            queries[:, h * KEY_DIM : (h + 1) * KEY_DIM].astype(jnp.float32), cosine, sine
        ).astype(jnp.bfloat16)
        columns = slice(h * VALUE_DIM, (h + 1) * VALUE_DIM)
        gaps = cumulative[h][:, None] - cumulative[h][None, :]
        weight = jnp.where(causal, jnp.exp(jnp.minimum(gaps, 0.0)), 0.0)
        scores = lax.dot_general(
            query, head_keys[h], (((1,), (1,)), ((), ())), preferred_element_type=jnp.float32
        )
        decayed = (scores * weight).astype(jnp.bfloat16)
        within = jnp.dot(decayed, values[:, columns], preferred_element_type=jnp.float32)
        scaled = (query.astype(jnp.float32) * jnp.exp(cumulative[h])[:, None]).astype(jnp.bfloat16)
        retained = within + jnp.dot(scaled, incoming[h], preferred_element_type=jnp.float32)
        normed_head = layer_norm(retained, head_gain[columns])
        gated.append(
            (jax.nn.silu(gates[:, columns].astype(jnp.float32)) * normed_head).astype(jnp.bfloat16)
        )
    gated = jnp.concatenate(gated, axis=1)
    terms = jnp.dot(gated, output_weight, preferred_element_type=jnp.float32).astype(jnp.bfloat16)
    return scatter_sum(
        [terms[m * own_rows : (m + 1) * own_rows] for m in range(tp_count)], tp_count
    )


def expert_mixture(
    expert_input,
    expert_gain,
    routes,
    group_weight,
    pair_weight,
    expert_gate,
    expert_up,
    expert_down,
):
    tokens, width = expert_input.shape
    count = lax.axis_size("ep") * lax.axis_size("tp")
    plane = count // GROUPS
    capacity = 3 * tokens * TOPK // (2 * count)
    slots = plane * capacity // TOPK
    me = lax.axis_index("ep") * lax.axis_size("tp") + lax.axis_index("tp")
    my_plane = me // plane
    my_place = me % plane

    def to_plane(array, step):
        pairs = [
            (d, (d // plane + step) % GROUPS * plane + d % plane) for d in range(count)
        ]
        return lax.ppermute(array, AXES, pairs)

    def in_plane(array, mask):
        return lax.ppermute(array, AXES, [(d, d ^ mask) for d in range(count)])

    normed = layer_norm(expert_input, expert_gain).astype(jnp.bfloat16)
    group = routes[:, 0] // plane
    before = jnp.arange(tokens)[:, None] < jnp.arange(tokens)[None, :]
    group_rank = jnp.sum(
        (before & (group[:, None] == group[None, :])).astype(jnp.int32), axis=0
    )
    after = jnp.arange(tokens)[:, None] > jnp.arange(tokens)[None, :]
    mixing = group_weight[:, None] * pair_weight
    details = []
    for k in range(TOPK):
        mine = routes[:, k]
        hits = jnp.zeros((tokens, tokens), jnp.bool_)
        for other in range(TOPK):
            hits = hits | (mine[:, None] == routes[:, other][None, :])
        rank = jnp.sum((hits & after).astype(jnp.int32), axis=1)
        target = (mine - group * plane) * capacity + rank + 1
        share = mixing[:, k]
        high = share.astype(jnp.bfloat16)
        low = (share - high.astype(jnp.float32)).astype(jnp.bfloat16)
        details += [target.astype(jnp.bfloat16), high, low]
    details = jnp.stack(details, axis=1)
    details = jnp.pad(details, ((0, 0), (0, META - details.shape[1])))
    rows = jnp.concatenate([normed, details], axis=1)

    step_of = (group - my_plane + GROUPS) % GROUPS
    place = step_of * slots + group_rank
    choose = (
        jnp.arange(GROUPS * slots, dtype=jnp.int32)[:, None] == place[None, :]
    ).astype(jnp.bfloat16)
    packed = jnp.dot(choose, rows, preferred_element_type=jnp.float32).astype(jnp.bfloat16)
    relayed = [packed[:slots]]
    for step in range(1, GROUPS):
        relayed.append(to_plane(packed[step * slots : (step + 1) * slots], step))
    relayed = jnp.concatenate(relayed, axis=0)

    meta = relayed[:, width : width + 3 * TOPK].astype(jnp.float32)
    block = capacity * GROUPS
    source = jnp.arange(GROUPS * slots, dtype=jnp.int32) // slots
    lane = jnp.arange(plane * block, dtype=jnp.int32)[None, :]
    spread = jnp.zeros((GROUPS * slots, plane * block), jnp.bool_)
    high = jnp.zeros(spread.shape, jnp.float32)
    low = jnp.zeros(spread.shape, jnp.float32)
    for k in range(TOPK):
        target = meta[:, 3 * k].astype(jnp.int32) - 1
        there = (target // capacity ^ my_place) * block + source * capacity + target % capacity
        there = jnp.where(target >= 0, there, -1)
        hit = lane == there[:, None]
        spread = spread | hit
        high = high + jnp.where(hit, meta[:, 3 * k + 1][:, None], 0.0)
        low = low + jnp.where(hit, meta[:, 3 * k + 2][:, None], 0.0)
    sent = lax.dot_general(
        spread.astype(jnp.bfloat16),
        relayed[:, :width],
        (((0,), (0,)), ((), ())),
        preferred_element_type=jnp.float32,
    ).astype(jnp.bfloat16)
    arrived = [sent[:block]]
    for mask in range(1, plane):
        arrived.append(in_plane(sent[mask * block : (mask + 1) * block], mask))
    arrived = jnp.concatenate(arrived, axis=0)

    gate_part = jnp.dot(arrived, expert_gate[0], preferred_element_type=jnp.float32)
    up_part = jnp.dot(arrived, expert_up[0], preferred_element_type=jnp.float32)
    hidden = (jax.nn.silu(gate_part) * up_part).astype(jnp.bfloat16)
    result = jnp.dot(hidden, expert_down[0], preferred_element_type=jnp.float32).astype(
        jnp.bfloat16
    )

    returned = [result[:block]]
    for mask in range(1, plane):
        returned.append(in_plane(result[mask * block : (mask + 1) * block], mask))
    returned = jnp.concatenate(returned, axis=0)
    combined = (
        jnp.dot(high.astype(jnp.bfloat16), returned, preferred_element_type=jnp.float32)
        + jnp.dot(low.astype(jnp.bfloat16), returned, preferred_element_type=jnp.float32)
    ).astype(jnp.bfloat16)
    final = [combined[:slots]]
    for step in range(1, GROUPS):
        final.append(to_plane(combined[step * slots : (step + 1) * slots], GROUPS - step))
    final = jnp.concatenate(final, axis=0)
    return lax.dot_general(
        choose, final, (((0,), (0,)), ((), ())), preferred_element_type=jnp.float32
    ).astype(jnp.bfloat16)


def local(
    mixer_input,
    log_decay,
    mixer_gain,
    query_weight,
    key_weight,
    value_weight,
    gate_weight,
    head_gain,
    output_weight,
    expert_input,
    expert_gain,
    routes,
    group_weight,
    pair_weight,
    expert_gate,
    expert_up,
    expert_down,
):
    expert_output = expert_mixture(
        expert_input,
        expert_gain,
        routes,
        group_weight,
        pair_weight,
        expert_gate,
        expert_up,
        expert_down,
    )
    mixer_output = token_mixer(
        mixer_input,
        log_decay,
        mixer_gain,
        query_weight,
        key_weight,
        value_weight,
        gate_weight,
        head_gain,
        output_weight,
    )
    return (mixer_output, expert_output)


def solution(mesh):
    return jax.shard_map(
        local,
        mesh=mesh,
        in_specs=(
            P(("ep", "tp"), None),
            P("ep", "tp"),
            P(),
            P(None, "tp"),
            P(None, "tp"),
            P(None, "tp"),
            P(None, "tp"),
            P("tp"),
            P("tp", None),
            P(("ep", "tp"), None),
            P(),
            P(("ep", "tp"), None),
            P(("ep", "tp")),
            P(("ep", "tp"), None),
            P(("ep", "tp"), None, None),
            P(("ep", "tp"), None, None),
            P(("ep", "tp"), None, None),
        ),
        out_specs=(P(("ep", "tp"), None), P(("ep", "tp"), None)),
        check_vma=False,
    )
```

```python
import jax
import jax.numpy as jnp
from jax import lax
from jax.sharding import PartitionSpec as P


KEY_DIM = 128
VALUE_DIM = 256
TOPK = 2
GROUPS = 4
META = 128

EPSILON = 1e-05
THETA = 10000.0
AXES = ("ep", "tp")


def layer_norm(matrix, norm_gain):
    matrix = matrix.astype(jnp.float32)
    average = jnp.mean(matrix, axis=-1, keepdims=True)
    centred = matrix - average
    spread = jnp.mean(centred * centred, axis=-1, keepdims=True)
    return centred * lax.rsqrt(spread + EPSILON) * norm_gain


def rotate(values, cosine, sine):
    halfway = values.shape[-1] // 2
    leading = values[..., :halfway]
    trailing = values[..., halfway:]
    return jnp.concatenate(
        [leading * cosine - trailing * sine, trailing * cosine + leading * sine], axis=-1
    )


def flip(array, axis, count, mask):
    return lax.ppermute(array, axis, [(i, i ^ mask) for i in range(count)])


def later(array, count, step):
    return lax.ppermute(array, "ep", [(i, i + step) for i in range(count - step)])


def gather_rows(rows, tp_count):
    blocks = [rows] * tp_count
    for far in range(2, tp_count, 2):
        blocks[far] = flip(rows, "tp", tp_count, far)
    blocks[1] = flip(rows, "tp", tp_count, 1)
    for far in range(2, tp_count, 2):
        blocks[far + 1] = flip(blocks[far], "tp", tp_count, 1)
    return blocks


def scatter_sum(blocks, tp_count):
    total = blocks[0].astype(jnp.float32)
    pairs = [
        flip(blocks[far + 1], "tp", tp_count, 1) for far in range(2, tp_count, 2)
    ]
    partner = flip(blocks[1], "tp", tp_count, 1)
    arrived = []
    for place, far in enumerate(range(2, tp_count, 2)):
        both = blocks[far].astype(jnp.float32) + pairs[place].astype(jnp.float32)
        arrived.append(flip(both.astype(jnp.bfloat16), "tp", tp_count, far))
    total = total + partner.astype(jnp.float32)
    for part in arrived:
        total = total + part.astype(jnp.float32)
    return total.astype(jnp.bfloat16)


def token_mixer(
    mixer_input,
    log_decay,
    mixer_gain,
    query_weight,
    key_weight,
    value_weight,
    gate_weight,
    head_gain,
    output_weight,
):
    ep_count = lax.axis_size("ep")
    tp_count = lax.axis_size("tp")
    place = lax.axis_index("tp")
    own_rows = mixer_input.shape[0]
    seg_rows = own_rows * tp_count
    heads_dev = query_weight.shape[1] // KEY_DIM

    normed = layer_norm(mixer_input, mixer_gain).astype(jnp.bfloat16)
    gathered = jnp.concatenate(gather_rows(normed, tp_count), axis=0)
    gathered = yield gathered

    row = jnp.arange(seg_rows, dtype=jnp.int32)
    offset = (row // own_rows ^ place) * own_rows + row % own_rows
    natural = jnp.arange(seg_rows, dtype=jnp.int32)
    reach = (natural[None, :] <= offset[:, None])
    causal = offset[:, None] >= offset[None, :]
    cumulative = [
        jnp.sum(jnp.where(reach, log_decay[:, h][None, :], 0.0), axis=1)
        for h in range(heads_dev)
    ]
    totals = jnp.sum(log_decay, axis=0)

    position = (lax.axis_index("ep") * seg_rows + offset).astype(jnp.float32)
    halfway = KEY_DIM // 2
    frequency = THETA ** (-jnp.arange(halfway, dtype=jnp.float32) / halfway)
    angles = position[:, None] * frequency[None, :]
    cosine = jnp.cos(angles)
    sine = jnp.sin(angles)

    def project(weight):
        return jnp.dot(gathered, weight, preferred_element_type=jnp.float32)

    keys = project(key_weight).astype(jnp.bfloat16)
    values = project(value_weight).astype(jnp.bfloat16)
    queries = project(query_weight).astype(jnp.bfloat16)
    gates = project(gate_weight).astype(jnp.bfloat16)

    states = []
    head_keys = []
    for h in range(heads_dev):
        key = rotate(
            keys[:, h * KEY_DIM : (h + 1) * KEY_DIM].astype(jnp.float32), cosine, sine
        ).astype(jnp.bfloat16)
        head_keys.append(key)
        remain = jnp.exp(totals[h] - cumulative[h])
        weighted = (key.astype(jnp.float32) * remain[:, None]).astype(jnp.bfloat16)
        states.append(
            lax.dot_general(
                weighted,
                values[:, h * VALUE_DIM : (h + 1) * VALUE_DIM],
                (((0,), (0,)), ((), ())),
                preferred_element_type=jnp.float32,
            )
        )
    states = yield states

    def pack(window, parts):
        high = window.astype(jnp.bfloat16)
        rest = window - high.astype(jnp.float32)
        middle = rest.astype(jnp.bfloat16)
        low = (rest - middle.astype(jnp.float32)).astype(jnp.bfloat16)
        extra = jnp.stack([high, middle, low], axis=0).reshape(-1, 1)
        extra = jnp.pad(extra, ((0, 16 - extra.shape[0]), (0, VALUE_DIM - 1)))
        return jnp.concatenate([part.astype(jnp.bfloat16) for part in parts] + [extra], axis=0)

    def unpack(packed):
        parts = [
            packed[h * KEY_DIM : (h + 1) * KEY_DIM].astype(jnp.float32) for h in range(heads_dev)
        ]
        first = heads_dev * KEY_DIM
        terms = packed[first : first + 3 * heads_dev, 0].astype(jnp.float32)
        return jnp.sum(terms.reshape(3, heads_dev), axis=0), parts

    def join(near, far):
        return near[0] + far[0], [
            part + jnp.exp(near[0][h]) * far[1][h] for h, part in enumerate(near[1])
        ]

    packed = pack(totals, states)
    incoming = unpack(later(packed, ep_count, 1))
    covered = 1
    if ep_count > 2:
        incoming = join(incoming, unpack(later(packed, ep_count, 2)))
        covered = 2
    window, parts = incoming
    parts = yield parts
    incoming = (window, parts)
    while covered < ep_count - 1:
        incoming = join(incoming, unpack(later(pack(*incoming), ep_count, covered)))
        covered *= 2
    incoming = [part.astype(jnp.bfloat16) for part in incoming[1]]
    queries = yield queries

    gated = []
    for h in range(heads_dev):
        query = rotate(
            queries[:, h * KEY_DIM : (h + 1) * KEY_DIM].astype(jnp.float32), cosine, sine
        ).astype(jnp.bfloat16)
        columns = slice(h * VALUE_DIM, (h + 1) * VALUE_DIM)
        gaps = cumulative[h][:, None] - cumulative[h][None, :]
        weight = jnp.where(causal, jnp.exp(jnp.minimum(gaps, 0.0)), 0.0)
        scores = lax.dot_general(
            query, head_keys[h], (((1,), (1,)), ((), ())), preferred_element_type=jnp.float32
        )
        decayed = (scores * weight).astype(jnp.bfloat16)
        within = jnp.dot(decayed, values[:, columns], preferred_element_type=jnp.float32)
        scaled = (query.astype(jnp.float32) * jnp.exp(cumulative[h])[:, None]).astype(jnp.bfloat16)
        retained = within + jnp.dot(scaled, incoming[h], preferred_element_type=jnp.float32)
        normed_head = layer_norm(retained, head_gain[columns])
        gated.append(
            (jax.nn.silu(gates[:, columns].astype(jnp.float32)) * normed_head).astype(jnp.bfloat16)
        )
    gated = jnp.concatenate(gated, axis=1)
    terms = jnp.dot(gated, output_weight, preferred_element_type=jnp.float32).astype(jnp.bfloat16)
    terms = yield terms
    yield scatter_sum(
        [terms[m * own_rows : (m + 1) * own_rows] for m in range(tp_count)], tp_count
    )


def expert_mixture(
    expert_input,
    expert_gain,
    routes,
    group_weight,
    pair_weight,
    expert_gate,
    expert_up,
    expert_down,
):
    tokens, width = expert_input.shape
    count = lax.axis_size("ep") * lax.axis_size("tp")
    plane = count // GROUPS
    capacity = 3 * tokens * TOPK // (2 * count)
    slots = plane * capacity // TOPK
    me = lax.axis_index("ep") * lax.axis_size("tp") + lax.axis_index("tp")
    my_plane = me // plane
    my_place = me % plane

    def to_plane(array, step):
        pairs = [
            (d, (d // plane + step) % GROUPS * plane + d % plane) for d in range(count)
        ]
        return lax.ppermute(array, AXES, pairs)

    def in_plane(array, mask):
        return lax.ppermute(array, AXES, [(d, d ^ mask) for d in range(count)])

    normed = layer_norm(expert_input, expert_gain).astype(jnp.bfloat16)
    group = routes[:, 0] // plane
    before = jnp.arange(tokens)[:, None] < jnp.arange(tokens)[None, :]
    group_rank = jnp.sum(
        (before & (group[:, None] == group[None, :])).astype(jnp.int32), axis=0
    )
    after = jnp.arange(tokens)[:, None] > jnp.arange(tokens)[None, :]
    mixing = group_weight[:, None] * pair_weight
    details = []
    for k in range(TOPK):
        mine = routes[:, k]
        hits = jnp.zeros((tokens, tokens), jnp.bool_)
        for other in range(TOPK):
            hits = hits | (mine[:, None] == routes[:, other][None, :])
        rank = jnp.sum((hits & after).astype(jnp.int32), axis=1)
        target = (mine - group * plane) * capacity + rank + 1
        share = mixing[:, k]
        high = share.astype(jnp.bfloat16)
        low = (share - high.astype(jnp.float32)).astype(jnp.bfloat16)
        details += [target.astype(jnp.bfloat16), high, low]
    details = jnp.stack(details, axis=1)
    details = jnp.pad(details, ((0, 0), (0, META - details.shape[1])))
    rows = jnp.concatenate([normed, details], axis=1)

    step_of = (group - my_plane + GROUPS) % GROUPS
    place = step_of * slots + group_rank
    choose = (
        jnp.arange(GROUPS * slots, dtype=jnp.int32)[:, None] == place[None, :]
    ).astype(jnp.bfloat16)
    packed = jnp.dot(choose, rows, preferred_element_type=jnp.float32).astype(jnp.bfloat16)
    relayed = [packed[:slots]]
    for step in range(1, GROUPS):
        relayed.append(to_plane(packed[step * slots : (step + 1) * slots], step))
    relayed = jnp.concatenate(relayed, axis=0)

    meta = relayed[:, width : width + 3 * TOPK].astype(jnp.float32)
    block = capacity * GROUPS
    source = jnp.arange(GROUPS * slots, dtype=jnp.int32) // slots
    lane = jnp.arange(plane * block, dtype=jnp.int32)[None, :]
    spread = jnp.zeros((GROUPS * slots, plane * block), jnp.bool_)
    high = jnp.zeros(spread.shape, jnp.float32)
    low = jnp.zeros(spread.shape, jnp.float32)
    for k in range(TOPK):
        target = meta[:, 3 * k].astype(jnp.int32) - 1
        there = (target // capacity ^ my_place) * block + source * capacity + target % capacity
        there = jnp.where(target >= 0, there, -1)
        hit = lane == there[:, None]
        spread = spread | hit
        high = high + jnp.where(hit, meta[:, 3 * k + 1][:, None], 0.0)
        low = low + jnp.where(hit, meta[:, 3 * k + 2][:, None], 0.0)
    sent = lax.dot_general(
        spread.astype(jnp.bfloat16),
        relayed[:, :width],
        (((0,), (0,)), ((), ())),
        preferred_element_type=jnp.float32,
    ).astype(jnp.bfloat16)
    sent = yield sent
    arrived = [sent[:block]]
    for mask in range(1, plane):
        arrived.append(in_plane(sent[mask * block : (mask + 1) * block], mask))
    arrived = jnp.concatenate(arrived, axis=0)
    arrived = yield arrived

    gate_part = jnp.dot(arrived, expert_gate[0], preferred_element_type=jnp.float32)
    gate_part = yield gate_part
    up_part = jnp.dot(arrived, expert_up[0], preferred_element_type=jnp.float32)
    hidden = (jax.nn.silu(gate_part) * up_part).astype(jnp.bfloat16)
    result = jnp.dot(hidden, expert_down[0], preferred_element_type=jnp.float32).astype(
        jnp.bfloat16
    )

    result = yield result
    returned = [result[:block]]
    for mask in range(1, plane):
        returned.append(in_plane(result[mask * block : (mask + 1) * block], mask))
    returned = jnp.concatenate(returned, axis=0)
    returned = yield returned
    combined = (
        jnp.dot(high.astype(jnp.bfloat16), returned, preferred_element_type=jnp.float32)
        + jnp.dot(low.astype(jnp.bfloat16), returned, preferred_element_type=jnp.float32)
    ).astype(jnp.bfloat16)
    final = [combined[:slots]]
    for step in range(1, GROUPS):
        final.append(to_plane(combined[step * slots : (step + 1) * slots], GROUPS - step))
    final = jnp.concatenate(final, axis=0)
    yield lax.dot_general(
        choose, final, (((0,), (0,)), ((), ())), preferred_element_type=jnp.float32
    ).astype(jnp.bfloat16)


def local(
    mixer_input,
    log_decay,
    mixer_gain,
    query_weight,
    key_weight,
    value_weight,
    gate_weight,
    head_gain,
    output_weight,
    expert_input,
    expert_gain,
    routes,
    group_weight,
    pair_weight,
    expert_gate,
    expert_up,
    expert_down,
):
    experts = expert_mixture(
        expert_input,
        expert_gain,
        routes,
        group_weight,
        pair_weight,
        expert_gate,
        expert_up,
        expert_down,
    )
    mixer = token_mixer(
        mixer_input,
        log_decay,
        mixer_gain,
        query_weight,
        key_weight,
        value_weight,
        gate_weight,
        head_gain,
        output_weight,
    )
    ours = next(experts)
    theirs = next(mixer)
    for mixer_waits in (True, False, False, True, False):
        after, before = lax.optimization_barrier((ours, theirs))
        if mixer_waits:
            theirs = before
        else:
            ours = after
        ours = experts.send(ours)
        theirs = mixer.send(theirs)
    return (theirs, ours)


def solution(mesh):
    return jax.shard_map(
        local,
        mesh=mesh,
        in_specs=(
            P(("ep", "tp"), None),
            P("ep", "tp"),
            P(),
            P(None, "tp"),
            P(None, "tp"),
            P(None, "tp"),
            P(None, "tp"),
            P("tp"),
            P("tp", None),
            P(("ep", "tp"), None),
            P(),
            P(("ep", "tp"), None),
            P(("ep", "tp")),
            P(("ep", "tp"), None),
            P(("ep", "tp"), None, None),
            P(("ep", "tp"), None, None),
            P(("ep", "tp"), None, None),
        ),
        out_specs=(P(("ep", "tp"), None), P(("ep", "tp"), None)),
        check_vma=False,
    )
```
